32 devices in a mesh: sp: 4 (over z), fs: 4 (over y, x), tp: 2 (over core).
Axes of the slice: x: 2, y: 2, z: 4, core: 2. Of those that a mesh axis runs over, the one named last changes fastest.
Arguments:
- tokens: bfloat16 [4, 3072, 2048], P('fs', 'sp'), may hold values from -6 to 6
- norm_gain: float32 [2048], replicated, may hold values from 0.1 to 1.9
- query_weight: bfloat16 [2048, 512], P(('sp', 'fs'), 'tp'), may hold values from -0.125 to 0.125
- key_weight: bfloat16 [2048, 512], P(('sp', 'fs'), 'tp'), may hold values from -0.125 to 0.125
- value_weight: bfloat16 [2048, 1024], P(('sp', 'fs'), 'tp'), may hold values from -0.125 to 0.125
- gate_weight: bfloat16 [2048, 1024], P(('sp', 'fs'), 'tp'), may hold values from -0.125 to 0.125
- conv_b_weight: bfloat16 [2048, 1024], P(('sp', 'fs'), 'tp'), may hold values from -0.125 to 0.125
- conv_c_weight: bfloat16 [2048, 1024], P(('sp', 'fs'), 'tp'), may hold values from -0.125 to 0.125
- conv_in_weight: bfloat16 [2048, 1024], P(('sp', 'fs'), 'tp'), may hold values from -0.125 to 0.125
- conv_kernel: float32 [3, 1024], P(None, 'tp'), may hold values from -3.5 to 3.5
- out_ret_weight: bfloat16 [2048, 1024], P(('sp', 'fs'), 'tp'), may hold values from -0.125 to 0.125
- out_conv_weight: bfloat16 [2048, 1024], P(('sp', 'fs'), 'tp'), may hold values from -0.125 to 0.125
- log_decay: float32 [4, 8, 3072], P('fs', 'tp', 'sp'), may hold values from -3 to 0, as said below
Outputs:
- mixed: bfloat16 [4, 3072, 2048], P('fs', ('sp', 'tp'))
The draws below stay inside these ranges and needn't reach their ends.
Inputs may be any that keep to these rules, and one draw needn't show every extreme that they name: log_decay is never positive.
All inputs are finite; a program needn't handle non-finite values.
Results may differ from the reference program's by a relative error of at most 0.02.
Values may be sent and summed in bfloat16 or wider, within the bound.
A program may use at most 64 MiB of HBM per device.

```python
import jax
import jax.numpy as jnp
from jax import lax

MODEL = 2048
MEMORY_CHANNELS = 8
KEY_DIM = 64
VALUE_DIM = 128
CONV_DIM = 1024
CONV_TAPS = 3
BLOCK_LEN = 128
TOK_DEV = 768
SERIES_NUMBER = 4
SERIES_SPAN = 3072
N_TP = 2


def draw_log_decay(key, part):
    lookup_matrix_lines = jax.random.split(jax.random.fold_in(key, 17), 7)
    head_shape = (SERIES_NUMBER, MEMORY_CHANNELS, 1)
    fast_share = 0.5
    is_fast = jax.random.uniform(lookup_matrix_lines[0], head_shape, jnp.float32) < fast_share
    fast_rate = jnp.exp(jax.random.uniform(lookup_matrix_lines[1], head_shape, jnp.float32, jnp.log(0.04), jnp.log(0.1)))
    slow_rate = jnp.exp(jax.random.uniform(lookup_matrix_lines[2], head_shape, jnp.float32, jnp.log(0.1), jnp.log(0.25))) / SERIES_SPAN
    background_frequency = jnp.where(is_fast, fast_rate, slow_rate)
    segment_multiplier = jnp.exp(jax.random.uniform(lookup_matrix_lines[3], (SERIES_NUMBER, MEMORY_CHANNELS, SERIES_SPAN // TOK_DEV), jnp.float32, -0.7, 0.7))
    segment_multiplier = jnp.repeat(segment_multiplier, TOK_DEV, axis=-1)
    noise_magnitude = jax.random.uniform(lookup_matrix_lines[4], (SERIES_NUMBER, MEMORY_CHANNELS, SERIES_SPAN), jnp.float32, 0.4, 1.6)
    spike_places = jax.random.randint(lookup_matrix_lines[5], (SERIES_NUMBER, MEMORY_CHANNELS, 3), 0, SERIES_SPAN)
    spike_magnitude = jnp.log(jax.random.uniform(lookup_matrix_lines[6], (SERIES_NUMBER, MEMORY_CHANNELS, 3), jnp.float32, 0.55, 0.8))
    token_ordinal = jnp.arange(SERIES_SPAN)
    spike_occurrences = jnp.sum(jnp.where(token_ordinal[None, None, :, None] == spike_places[:, :, None, :], spike_magnitude[:, :, None, :], 0.0), axis=-1)
    return (spike_occurrences - background_frequency * segment_multiplier * noise_magnitude).astype(jnp.float32)


def block_levels(rng, extent, pieces, smallest, top_value):
    gain, own = 1.0, jax.random.fold_in(rng, 6)
    for axis_at, shards_of in pieces:
        draws = jnp.exp(jax.random.uniform(jax.random.fold_in(own, axis_at), (shards_of,), jnp.float32, smallest / len(pieces), top_value / len(pieces)))
        gain = gain * jnp.repeat(draws, extent[axis_at] // shards_of).reshape([-1 if axis == axis_at else 1 for axis in range(len(extent))])
    return gain


def noise(stream_key, dims, width, bound, cuts=(), kind=jnp.bfloat16):
    values = jax.random.normal(stream_key, dims, jnp.float32) * width
    if len(cuts) > 0:
        values = block_levels(stream_key, dims, cuts, -0.22, 0.18) * values
    return jnp.clip(values, min=-bound, max=bound).astype(kind)


def setup_inputs(seed: int = 0) -> dict:
    keys = jax.random.split(jax.random.key(seed), 14)
    return {
        "tokens": noise(keys[0], (SERIES_NUMBER, SERIES_SPAN, MODEL), 1.0, 6.0, ((0, 4), (1, 4))),
        "norm_gain": jnp.clip(1.0 + 0.18 * jax.random.normal(keys[1], (MODEL,), jnp.float32), 0.1, 1.9),
        "query_weight": noise(keys[2], (MODEL, MEMORY_CHANNELS * KEY_DIM), MODEL ** -0.5, 0.125, ((0, 16), (1, 2))),
        "key_weight": noise(keys[3], (MODEL, MEMORY_CHANNELS * KEY_DIM), MODEL ** -0.5, 0.125, ((0, 16), (1, 2))),
        "value_weight": noise(keys[4], (MODEL, MEMORY_CHANNELS * VALUE_DIM), MODEL ** -0.5, 0.125, ((0, 16), (1, 2))),
        "gate_weight": noise(keys[5], (MODEL, MEMORY_CHANNELS * VALUE_DIM), MODEL ** -0.5, 0.125, ((0, 16), (1, 2))),
        "conv_b_weight": noise(keys[6], (MODEL, CONV_DIM), MODEL ** -0.5, 0.125, ((0, 16), (1, 2))),
        "conv_c_weight": noise(keys[7], (MODEL, CONV_DIM), MODEL ** -0.5, 0.125, ((0, 16), (1, 2))),
        "conv_in_weight": noise(keys[8], (MODEL, CONV_DIM), MODEL ** -0.5, 0.125, ((0, 16), (1, 2))),
        "conv_kernel": noise(keys[9], (CONV_TAPS, CONV_DIM), CONV_TAPS ** -0.5, 3.5, ((1, 2),), jnp.float32),
        "out_ret_weight": noise(keys[10], (MODEL, MEMORY_CHANNELS * VALUE_DIM), (MEMORY_CHANNELS * VALUE_DIM + CONV_DIM) ** -0.5, 0.125, ((0, 16), (1, 2))),
        "out_conv_weight": noise(keys[11], (MODEL, CONV_DIM), (MEMORY_CHANNELS * VALUE_DIM + CONV_DIM) ** -0.5, 0.125, ((0, 16), (1, 2))),
        "log_decay": draw_log_decay(jax.random.fold_in(keys[13], 71), 0),
    }


EPSILON = 1e-06
ROPE_BASE = 10000.0

def to_half(values):
    return lax.optimization_barrier(values.astype(jnp.bfloat16))

def rotate(values, token_ordinal):
    half_dim = values.shape[-1] // 2
    frequency = 1.0 / ROPE_BASE ** jnp.linspace(0.0, 1.0, half_dim, dtype=jnp.float32)
    angles = token_ordinal[:, None] * frequency[None, :]
    cosine_table = jnp.cos(angles)[:, None, :]
    sine_table = jnp.sin(angles)[:, None, :]
    first = values[..., :half_dim].astype(jnp.float32)
    second = values[..., half_dim:].astype(jnp.float32)
    return jnp.concatenate([first * cosine_table - second * sine_table, first * sine_table + second * cosine_table], axis=-1)

def retention_pass(queries, lookup_matrix_lines, values, decays):
    length, head_count, key_dim = queries.shape
    blocks = length // BLOCK_LEN

    def split_blocks(array):
        shaped = array.reshape(blocks, BLOCK_LEN, head_count, array.shape[-1])
        return jnp.transpose(shaped, (0, 2, 1, 3)).astype(jnp.float32)
    query_blocks = split_blocks(queries)
    key_blocks = split_blocks(lookup_matrix_lines)
    value_blocks = split_blocks(values)
    decay_blocks = jnp.transpose(decays.reshape(head_count, blocks, BLOCK_LEN), (1, 0, 2))
    cumulative = jnp.cumsum(decay_blocks, axis=-1)
    ending = cumulative[..., -1:]
    decay_gaps = cumulative[..., :, None] - cumulative[..., None, :]
    causal = jnp.arange(BLOCK_LEN)[:, None] >= jnp.arange(BLOCK_LEN)[None, :]
    weighting = jnp.where(causal, jnp.exp(jnp.minimum(decay_gaps, 0.0)), 0.0)
    scores = to_half(jnp.einsum('nhid,nhjd->nhij', query_blocks, key_blocks) * weighting).astype(jnp.float32)
    intra_out = jnp.einsum('nhij,nhje->nhie', scores, value_blocks)
    decayed_keys = to_half(key_blocks * jnp.exp(ending - cumulative)[..., None]).astype(jnp.float32)
    decayed_queries = to_half(query_blocks * jnp.exp(cumulative)[..., None]).astype(jnp.float32)
    block_kv = jnp.einsum('nhjd,nhje->nhde', decayed_keys, value_blocks)

    def advance(state_now, step_in):
        kv_block, total = step_in
        return (state_now * jnp.exp(total)[:, None, None] + kv_block, state_now)
    start_state = jnp.zeros((head_count, key_dim, values.shape[-1]), jnp.float32)
    _, before = lax.scan(advance, start_state, (block_kv, ending[..., 0]))
    cross = jnp.einsum('nhid,nhde->nhie', decayed_queries, to_half(before).astype(jnp.float32))
    output = intra_out + cross
    output = output * lax.rsqrt(lax.optimization_barrier(jnp.mean(output * output, axis=-1, keepdims=True)) + EPSILON)
    return jnp.transpose(output, (0, 2, 1, 3)).reshape(length, head_count * output.shape[-1])

def reference(tokens, norm_gain, query_weight, key_weight, value_weight, gate_weight, conv_b_weight, conv_c_weight, conv_in_weight, conv_kernel, out_ret_weight, out_conv_weight, log_decay):

    def one_sequence(pair):
        sequence_tokens, sequence_decay = pair
        inputs = sequence_tokens.astype(jnp.float32)
        length = inputs.shape[0]
        normed = to_half(inputs * lax.rsqrt(lax.optimization_barrier(jnp.mean(inputs * inputs, axis=-1, keepdims=True)) + EPSILON) * norm_gain.astype(jnp.float32))

        def project(weight):
            return to_half(jnp.dot(normed, weight, preferred_element_type=jnp.float32))
        token_ordinal = jnp.arange(length, dtype=jnp.float32)
        query_raw = project(query_weight).reshape(length, MEMORY_CHANNELS, KEY_DIM)
        key_raw = project(key_weight).reshape(length, MEMORY_CHANNELS, KEY_DIM)
        value_proj = project(value_weight).reshape(length, MEMORY_CHANNELS, VALUE_DIM)
        queries = to_half(rotate(query_raw, token_ordinal))
        lookup_matrix_lines = to_half(rotate(key_raw, token_ordinal) * KEY_DIM ** (-0.5))
        retained = retention_pass(queries, lookup_matrix_lines, value_proj, sequence_decay)
        ret_out = to_half(retained * jax.nn.silu(project(gate_weight).astype(jnp.float32)))
        gate_b = project(conv_b_weight).astype(jnp.float32)
        gate_c = project(conv_c_weight).astype(jnp.float32)
        conv_input = project(conv_in_weight).astype(jnp.float32)
        product = gate_c * conv_input
        padded = jnp.concatenate([jnp.zeros((CONV_TAPS - 1, CONV_DIM), jnp.float32), product], axis=0)
        convolved = jnp.zeros((length, CONV_DIM), jnp.float32)
        for tap_index in range(CONV_TAPS):
            convolved = convolved + conv_kernel[tap_index].astype(jnp.float32) * padded[tap_index:tap_index + length]
        conv_out = to_half(gate_b * convolved)
        ret_group = MEMORY_CHANNELS * VALUE_DIM // N_TP
        conv_group = CONV_DIM // N_TP
        total = jnp.zeros((length, MODEL), jnp.float32)
        for group in range(N_TP):
            ret_cols = slice(group * ret_group, (group + 1) * ret_group)
            conv_cols = slice(group * conv_group, (group + 1) * conv_group)
            partial_value = jnp.dot(ret_out[:, ret_cols], out_ret_weight[:, ret_cols].T, preferred_element_type=jnp.float32)
            partial_value = partial_value + jnp.dot(conv_out[:, conv_cols], out_conv_weight[:, conv_cols].T, preferred_element_type=jnp.float32)
            total = total + to_half(partial_value).astype(jnp.float32)
        return total.astype(jnp.bfloat16)
    return lax.map(one_sequence, (tokens, log_decay))
```

```python
import jax
import jax.numpy as jnp
from jax import lax
from jax.experimental import pallas as pl
from jax.experimental.pallas import tpu as pltpu
from jax.sharding import PartitionSpec as P

KEY_DIM = 64
VALUE_DIM = 128
CONV_TAPS = 3
BLOCK_LEN = 128


EPSILON = 1e-06
ROPE_BASE = 10000.0


def entering(x, axis, combine, identity):
    length, here = (lax.axis_size(axis), lax.axis_index(axis))
    everything = jax.tree.map(
        lambda part, kind: lax.all_gather(part.astype(kind), axis), x, (jnp.bfloat16, jnp.bfloat16)
    )
    start = jax.tree.map(
        lambda part, zero: jnp.broadcast_to(jnp.asarray(zero, part.dtype), part.shape), x, identity
    )

    def lap(k, before):
        reached = k < here
        new = combine(
            before, jax.tree.map(lambda part, own: part[k].astype(own.dtype), everything, x)
        )
        return jax.tree.map(lambda a, b: jnp.where(reached, a, b), new, before)

    return lax.fori_loop(0, length, lap, start)


def passed_along(value, axis, steps):
    count = lax.axis_size(axis)
    first, last = (max(0, -steps), min(count, count - steps))
    return lax.ppermute(value, axis, [(source, source + steps) for source in range(first, last)])


def rotate(values, token_ordinal):
    half_dim = values.shape[-1] // 2
    frequency = 1.0 / ROPE_BASE ** jnp.linspace(0.0, 1.0, half_dim, dtype=jnp.float32)
    angles = token_ordinal[:, None] * frequency[None, :]
    cosine_table = jnp.cos(angles)[:, None, :]
    sine_table = jnp.sin(angles)[:, None, :]
    first = values[..., :half_dim].astype(jnp.float32)
    second = values[..., half_dim:].astype(jnp.float32)
    return jnp.concatenate(
        [first * cosine_table - second * sine_table, first * sine_table + second * cosine_table],
        axis=-1,
    )


def make_adder(normed, contracted, pieces):
    updated = []
    for member in range(len(pieces)):
        portion = pieces[member]
        if member < contracted:
            updated.append(jnp.dot(normed, portion, preferred_element_type=jnp.float32))
        else:
            updated.append(portion)
    return tuple(updated)


def retention_local(projections, decays, token_ordinal):
    tok_rows = token_ordinal.shape[0]
    head_count = decays.shape[0]
    blocks = tok_rows // BLOCK_LEN
    query_raw = projections[0].reshape(tok_rows, head_count, KEY_DIM)
    key_raw = projections[1].reshape(tok_rows, head_count, KEY_DIM)
    queries = rotate(query_raw, token_ordinal).astype(jnp.bfloat16)
    lookup_matrix_lines = (rotate(key_raw, token_ordinal) * KEY_DIM ** (-0.5)).astype(jnp.bfloat16)
    value_proj = projections[2].reshape(tok_rows, head_count, VALUE_DIM)

    def split_blocks(array):
        shaped = array.reshape(blocks, BLOCK_LEN, head_count, array.shape[-1])
        return jnp.transpose(shaped, (0, 2, 1, 3))

    query_blocks = split_blocks(queries)
    key_blocks = split_blocks(lookup_matrix_lines)
    value_blocks = split_blocks(value_proj)
    decay_blocks = jnp.transpose(decays.reshape(head_count, blocks, BLOCK_LEN), (1, 0, 2))
    cumulative = jnp.cumsum(decay_blocks, axis=-1)
    ending = cumulative[..., -1:]
    decay_gaps = cumulative[..., :, None] - cumulative[..., None, :]
    causal = jnp.arange(BLOCK_LEN)[:, None] >= jnp.arange(BLOCK_LEN)[None, :]
    weighting = jnp.where(causal, jnp.exp(jnp.minimum(decay_gaps, 0.0)), 0.0)
    raw_scores = jnp.einsum(
        "nhid,nhjd->nhij", query_blocks, key_blocks, preferred_element_type=jnp.float32
    )
    scores = (raw_scores * weighting).astype(jnp.bfloat16)
    intra_out = jnp.einsum(
        "nhij,nhje->nhie", scores, value_blocks, preferred_element_type=jnp.float32
    )
    decayed_keys = (
        key_blocks.astype(jnp.float32) * jnp.exp(ending - cumulative)[..., None]
    ).astype(jnp.bfloat16)
    decayed_queries = (query_blocks.astype(jnp.float32) * jnp.exp(cumulative)[..., None]).astype(
        jnp.bfloat16
    )
    block_kv = jnp.einsum(
        "nhjd,nhje->nhde", decayed_keys, value_blocks, preferred_element_type=jnp.float32
    )
    block_ends = ending[..., 0]

    def advance(state_now, step_in):
        kv_block, total = step_in
        return (state_now * jnp.exp(total)[:, None, None] + kv_block, state_now)

    start_state = jnp.zeros((head_count, KEY_DIM, VALUE_DIM), jnp.float32)
    end_state, before_local = lax.scan(advance, start_state, (block_kv, block_ends))
    device_total = jnp.sum(block_ends, axis=0)
    return (intra_out, decayed_queries, before_local, block_ends, end_state, device_total)


def combine(earlier, later):
    return (earlier[0] * jnp.exp(later[1])[:, None, None] + later[0], earlier[1] + later[1])


def carried(end_state, device_total):
    identity = (jnp.zeros_like(end_state), jnp.zeros_like(device_total))
    state_in, _ = entering((end_state, device_total), "sp", combine, identity)
    return state_in


def retention_finish(local_parts, state_in, gate_proj):
    intra_out, decayed_queries, before_local, block_ends, end_state, device_total = local_parts
    starts = jnp.cumsum(block_ends, axis=0) - block_ends
    full_states = before_local + jnp.exp(starts)[:, :, None, None] * state_in[None]
    cross = jnp.einsum(
        "nhid,nhde->nhie",
        decayed_queries,
        full_states.astype(jnp.bfloat16),
        preferred_element_type=jnp.float32,
    )
    output = intra_out + cross
    output = output * lax.rsqrt(jnp.mean(output * output, axis=-1, keepdims=True) + EPSILON)
    tok_rows = gate_proj.shape[0]
    output = jnp.transpose(output, (0, 2, 1, 3)).reshape(tok_rows, gate_proj.shape[1])
    return (output * jax.nn.silu(gate_proj.astype(jnp.float32))).astype(jnp.bfloat16)


def convolve(conv_proj, conv_kernel):
    gate_b, gate_c, conv_input = conv_proj
    tok_rows = gate_b.shape[0]
    product = gate_c.astype(jnp.float32) * conv_input.astype(jnp.float32)
    rim_rows = passed_along(product[tok_rows - (CONV_TAPS - 1) :], "sp", 1)
    padded = jnp.concatenate([rim_rows, product], axis=0)
    convolved = jnp.zeros_like(product)
    for tap_index in range(CONV_TAPS):
        convolved = convolved + conv_kernel[tap_index] * padded[tap_index : tap_index + tok_rows]
    return (gate_b.astype(jnp.float32) * convolved).astype(jnp.bfloat16)


def shards(
    tokens,
    norm_gain,
    query_weight,
    key_weight,
    value_weight,
    gate_weight,
    conv_b_weight,
    conv_c_weight,
    conv_in_weight,
    conv_kernel,
    out_ret_weight,
    out_conv_weight,
    log_decay,
):
    inputs = tokens[0].astype(jnp.float32)
    tok_rows = inputs.shape[0]
    normed = (
        inputs * lax.rsqrt(jnp.mean(inputs * inputs, axis=-1, keepdims=True) + EPSILON) * norm_gain
    ).astype(jnp.bfloat16)
    token_ordinal = (
        lax.axis_index("sp") * tok_rows + jnp.arange(tok_rows, dtype=jnp.int32)
    ).astype(jnp.float32)
    decays = log_decay[0]
    gathered = make_adder(
        normed,
        7,
        (
            lax.all_gather(query_weight, ("sp", "fs"), axis=0, tiled=True),
            lax.all_gather(key_weight, ("sp", "fs"), axis=0, tiled=True),
            lax.all_gather(value_weight, ("sp", "fs"), axis=0, tiled=True),
            lax.all_gather(gate_weight, ("sp", "fs"), axis=0, tiled=True),
            lax.all_gather(conv_b_weight, ("sp", "fs"), axis=0, tiled=True),
            lax.all_gather(conv_c_weight, ("sp", "fs"), axis=0, tiled=True),
            lax.all_gather(conv_in_weight, ("sp", "fs"), axis=0, tiled=True),
            lax.all_gather(out_ret_weight, ("sp", "fs"), axis=0, tiled=True),
            lax.all_gather(out_conv_weight, ("sp", "fs"), axis=0, tiled=True),
        ),
    )
    ret_proj = [member.astype(jnp.bfloat16) for member in gathered[:4]]
    local_parts = retention_local(ret_proj, decays, token_ordinal)
    state_in = carried(local_parts[4], local_parts[5])
    conv_proj = [member.astype(jnp.bfloat16) for member in gathered[4:7]]
    full_ret, full_conv = (gathered[7], gathered[8])
    conv_out = convolve(conv_proj, conv_kernel)
    ret_out = retention_finish(local_parts, state_in, ret_proj[3])
    partial_value = lax.dot_general(
        ret_out, full_ret, (((1,), (1,)), ((), ())), preferred_element_type=jnp.float32
    )
    mixed = lax.psum_scatter(
        (
            partial_value
            + lax.dot_general(
                conv_out, full_conv, (((1,), (1,)), ((), ())), preferred_element_type=jnp.float32
            )
        ).astype(jnp.bfloat16),
        "tp",
        scatter_dimension=0,
        tiled=True,
    )
    return mixed[None]


MESH_IDS = pl.DeviceIdType.MESH


def remote(source, target, sent, landed, device):
    return pltpu.make_async_remote_copy(
        src_ref=source,
        dst_ref=target,
        send_sem=sent,
        recv_sem=landed,
        device_id=device,
        device_id_type=MESH_IDS,
    )


def greet(peers):
    barrier = pltpu.get_barrier_semaphore()
    for peer in peers:
        pl.semaphore_signal(barrier, inc=1, device_id=peer, device_id_type=MESH_IDS)
    pl.semaphore_wait(barrier, len(peers))


def plane_partners(f):
    x, y = f % 2, f // 2
    return y * 2 + (1 - x), (1 - y) * 2 + x, 3 - f


def gather_kernel(
    n_sp,
    half_ref,
    weight_ref,
    decay_ref,
    normed_ref,
    full_ref,
    decays_ref,
    norm_sent,
    norm_landed,
    side_sent,
    side_landed,
    relay_sent,
    weight_sent,
    weight_landed,
    up_sent,
    down_sent,
    line_landed,
    decay_sent,
    decay_landed,
    local_sem,
):
    s, f, t = lax.axis_index("sp"), lax.axis_index("fs"), lax.axis_index("tp")
    xn, yn, dn = plane_partners(f)
    half = half_ref.shape[0]
    chunk = half // 2
    rows = weight_ref.shape[1]
    n_fs = weight_ref.shape[0]
    other = {"tp": 1 - t}
    peers = [{"fs": xn}, {"fs": yn}, {"fs": dn}, other]
    peers += [{"sp": (s + d) % n_sp} for d in range(1, n_sp)]
    greet(peers)

    def spot(owner, core, piece):
        return normed_ref.at[owner, pl.ds(core * half + piece * chunk, chunk), :]

    def own(piece):
        return half_ref.at[pl.ds(piece * chunk, chunk), :]

    def block(b, g):
        return full_ref.at[pl.ds((b * n_fs + g) * rows, rows), :]

    waits = []
    locals_ = []

    def start(copy):
        copy.start()
        waits.append(copy)

    order = (xn, yn, dn)
    for i, p in enumerate(order):
        start(remote(weight_ref.at[p], block(s, f), weight_sent.at[i], weight_landed.at[f], {"fs": p}))
    for i, p in enumerate(order):
        start(remote(decay_ref.at[p], decays_ref.at[f], decay_sent.at[i], decay_landed.at[f], {"fs": p}))
    start(remote(own(0), spot(f, t, 0), norm_sent.at[0], norm_landed.at[f, 0], {"fs": xn}))
    start(remote(own(1), spot(f, t, 1), norm_sent.at[1], norm_landed.at[f, 1], {"fs": yn}))
    start(remote(own(1), spot(f, t, 1), norm_sent.at[2], norm_landed.at[f, 1], {"fs": xn}))
    start(remote(own(0), spot(f, t, 0), norm_sent.at[3], norm_landed.at[f, 0], {"fs": yn}))

    def line_copy(source, b, g, way):
        sent = up_sent if way == 1 else down_sent
        return remote(source, block(b, g), sent.at[b, g], line_landed.at[b, g], {"sp": s + way})

    def send_line(source, b, g):
        @pl.when(s < n_sp - 1)
        def _():
            line_copy(source, b, g, 1).start()

        @pl.when(s > 0)
        def _():
            line_copy(source, b, g, -1).start()

    send_line(weight_ref.at[f], s, f)
    for piece in range(2):
        start(remote(own(piece), spot(f, t, piece), side_sent.at[f, piece], side_landed.at[f, piece], other))
    for i, (a, b) in enumerate(
        (
            (own(0), spot(f, t, 0)),
            (own(1), spot(f, t, 1)),
            (weight_ref.at[f], block(s, f)),
            (decay_ref.at[f], decays_ref.at[f]),
        )
    ):
        copy = pltpu.make_async_copy(a, b, local_sem.at[i])
        copy.start()
        locals_.append(copy)

    for p in order:
        remote(weight_ref.at[p], block(s, p), weight_sent.at[0], weight_landed.at[p], {"fs": p}).wait_recv()
        send_line(block(s, p), s, p)

    def arrived(owner, piece):
        view = spot(owner, t, piece)
        remote(view, view, norm_sent.at[0], norm_landed.at[owner, piece], {"fs": owner}).wait_recv()
        start(remote(view, view, side_sent.at[owner, piece], side_landed.at[owner, piece], other))

    def line_step(d):
        for g in (f,) + order:

            @pl.when(s - d >= 0)
            def _():
                line_copy(block(s - d, g), s - d, g, 1).wait_recv()

                @pl.when(s < n_sp - 1)
                def _():
                    line_copy(block(s - d, g), s - d, g, 1).start()

            @pl.when(s + d <= n_sp - 1)
            def _():
                line_copy(block(s + d, g), s + d, g, -1).wait_recv()

                @pl.when(s > 0)
                def _():
                    line_copy(block(s + d, g), s + d, g, -1).start()

    arrived(xn, 0)
    start(remote(spot(xn, t, 0), spot(xn, t, 0), relay_sent.at[0], norm_landed.at[xn, 0], {"fs": yn}))
    arrived(yn, 1)
    start(remote(spot(yn, t, 1), spot(yn, t, 1), relay_sent.at[1], norm_landed.at[yn, 1], {"fs": xn}))
    line_step(1)
    arrived(xn, 1)
    arrived(yn, 0)
    for d in range(2, n_sp - 1):
        line_step(d)
    arrived(dn, 0)
    arrived(dn, 1)
    if n_sp > 2:
        line_step(n_sp - 1)
    for p in order:
        remote(decay_ref.at[p], decays_ref.at[p], decay_sent.at[0], decay_landed.at[p], {"fs": p}).wait_recv()
    for owner in range(n_fs):
        for piece in range(2):
            view = spot(owner, 1 - t, piece)
            remote(view, view, side_sent.at[0, 0], side_landed.at[owner, piece], other).wait_recv()
    for copy in waits:
        copy.wait_send()
    for copy in locals_:
        copy.wait()
    for b in range(n_sp):
        for g in range(n_fs):

            @pl.when((s < n_sp - 1) & (b <= s))
            def _():
                line_copy(block(b, g), b, g, 1).wait_send()

            @pl.when((s > 0) & (b >= s))
            def _():
                line_copy(block(b, g), b, g, -1).wait_send()


def gather_all(n_sp, half, pieces, decays):
    n_fs, rows, width = pieces.shape
    any_space = pl.BlockSpec(memory_space=pl.ANY)
    vmem = pl.BlockSpec(memory_space=pltpu.VMEM)
    dma = pltpu.SemaphoreType.DMA
    return pl.pallas_call(
        lambda *refs: gather_kernel(n_sp, *refs),
        out_shape=(
            jax.ShapeDtypeStruct((n_fs, 2 * half.shape[0], half.shape[1]), jnp.bfloat16),
            jax.ShapeDtypeStruct((n_sp * n_fs * rows, width), jnp.bfloat16),
            jax.ShapeDtypeStruct(decays.shape, jnp.float32),
        ),
        in_specs=[vmem] * 3,
        out_specs=(any_space, any_space, vmem),
        scratch_shapes=[
            dma((4,)),
            dma((n_fs, 2)),
            dma((n_fs, 2)),
            dma((n_fs, 2)),
            dma((2,)),
            dma((3,)),
            dma((n_fs,)),
            dma((n_sp, n_fs)),
            dma((n_sp, n_fs)),
            dma((n_sp, n_fs)),
            dma((3,)),
            dma((n_fs,)),
            dma((4,)),
        ],
        compiler_params=pltpu.CompilerParams(collective_id=0, has_side_effects=True),
        cost_estimate=pl.CostEstimate(flops=0, bytes_accessed=200_000_000, transcendentals=0),
        name="gather_all",
    )(half, pieces, decays)


def swap_kernel(
    mixed_ref, weight_ref, same_ref, cross_ref, far_ref, sent, same_landed, cross_landed, weight_sems, local_sem
):
    f, t = lax.axis_index("fs"), lax.axis_index("tp")
    half = same_ref.shape[1]
    order = plane_partners(f)
    peers = [{"fs": p, "tp": q} for p in order for q in (t, 1 - t)] + [{"tp": 1 - t}]
    greet(peers)

    def mine(p, core):
        return mixed_ref.at[p, pl.ds(core * half, half), :]

    copies = []
    for i, p in enumerate((order[2], order[0], order[1])):
        copies.append(
            remote(mine(p, t), same_ref.at[f], sent.at[2 * i], same_landed.at[f], {"fs": p})
        )
        copies.append(
            remote(
                mine(p, 1 - t),
                cross_ref.at[f],
                sent.at[2 * i + 1],
                cross_landed.at[f],
                {"fs": p, "tp": 1 - t},
            )
        )
    copies.append(remote(mine(f, 1 - t), cross_ref.at[f], sent.at[6], cross_landed.at[f], {"tp": 1 - t}))
    for copy in copies:
        copy.start()
    weight = remote(weight_ref, far_ref, weight_sems.at[0], weight_sems.at[1], {"tp": 1 - t})
    weight.start()
    local = pltpu.make_async_copy(mine(f, t), same_ref.at[f], local_sem)
    local.start()
    for p in order:
        remote(same_ref.at[p], same_ref.at[p], sent.at[0], same_landed.at[p], {"fs": p}).wait_recv()
    for p in order + (f,):
        remote(cross_ref.at[p], cross_ref.at[p], sent.at[0], cross_landed.at[p], {"tp": 1 - t}).wait_recv()
    for copy in copies:
        copy.wait_send()
    local.wait()
    weight.wait()


def swap(mixed, weight):
    n_fs, rows, width = mixed.shape
    any_space = pl.BlockSpec(memory_space=pl.ANY)
    vmem = pl.BlockSpec(memory_space=pltpu.VMEM)
    dma = pltpu.SemaphoreType.DMA
    piece = jax.ShapeDtypeStruct((n_fs, rows // 2, width), jnp.bfloat16)
    return pl.pallas_call(
        swap_kernel,
        out_shape=(piece, piece, jax.ShapeDtypeStruct(weight.shape, weight.dtype)),
        in_specs=[vmem, any_space],
        out_specs=(vmem, vmem, any_space),
        scratch_shapes=[dma((7,)), dma((n_fs,)), dma((n_fs,)), dma((2,)), dma],
        compiler_params=pltpu.CompilerParams(collective_id=1, has_side_effects=True),
        cost_estimate=pl.CostEstimate(flops=0, bytes_accessed=60_000_000, transcendentals=0),
        name="swap",
    )(mixed, weight)


def rotate_flat(values, cosine, sine):
    half_dim = values.shape[-1] // 2
    first = values[..., :half_dim].astype(jnp.float32)
    second = values[..., half_dim:].astype(jnp.float32)
    return jnp.concatenate([first * cosine - second * sine, first * sine + second * cosine], axis=-1)


def fast_shards(
    tokens,
    norm_gain,
    query_weight,
    key_weight,
    value_weight,
    gate_weight,
    conv_b_weight,
    conv_c_weight,
    conv_in_weight,
    conv_kernel,
    out_ret_weight,
    out_conv_weight,
    log_decay,
):
    n_sp, n_fs = lax.axis_size("sp"), lax.axis_size("fs")
    s, f, t = lax.axis_index("sp"), lax.axis_index("fs"), lax.axis_index("tp")
    tok_rows, model = tokens.shape[1:]
    half = tok_rows // 2
    blocks = tok_rows // BLOCK_LEN
    rows = query_weight.shape[0]
    inputs = lax.dynamic_slice_in_dim(tokens[0], t * half, half).astype(jnp.float32)
    normed = (
        inputs * lax.rsqrt(jnp.mean(inputs * inputs, axis=-1, keepdims=True) + EPSILON) * norm_gain
    ).astype(jnp.bfloat16)
    pieces = jnp.concatenate(
        [
            jnp.transpose(w.reshape(rows, n_fs, w.shape[1] // n_fs), (1, 0, 2))
            for w in (
                query_weight,
                key_weight,
                value_weight,
                gate_weight,
                conv_b_weight,
                conv_c_weight,
                conv_in_weight,
            )
        ],
        axis=-1,
    )
    own_out = jnp.concatenate([out_ret_weight, out_conv_weight], axis=-1)
    out_weight = lax.all_gather(own_out, ("sp", "fs"), axis=0, tiled=True)
    everyone, weights, decays = gather_all(
        n_sp, normed, pieces, log_decay[0].reshape(n_fs, blocks, BLOCK_LEN)
    )
    proj = jnp.dot(
        everyone.reshape(n_fs * tok_rows, model), weights, preferred_element_type=jnp.float32
    ).astype(jnp.bfloat16)
    proj = proj.reshape(n_fs, tok_rows, weights.shape[1])
    cuts = (KEY_DIM, 2 * KEY_DIM)
    q_raw, k_raw, wide = proj[..., : cuts[0]], proj[..., cuts[0] : cuts[1]], proj[..., cuts[1] :]
    values, ret_gate, gate_b, gate_c, conv_in = jnp.split(wide, 5, axis=-1)

    ordinal = (s * tok_rows + jnp.arange(tok_rows, dtype=jnp.int32)).astype(jnp.float32)
    frequency = 1.0 / ROPE_BASE ** jnp.linspace(0.0, 1.0, KEY_DIM // 2, dtype=jnp.float32)
    angles = ordinal[:, None] * frequency[None, :]
    cosine, sine = jnp.cos(angles), jnp.sin(angles)
    queries = rotate_flat(q_raw, cosine, sine).astype(jnp.bfloat16)
    keys = (rotate_flat(k_raw, cosine, sine) * KEY_DIM ** (-0.5)).astype(jnp.bfloat16)

    def cut(array):
        return array.reshape(n_fs, blocks, BLOCK_LEN, array.shape[-1])

    queries, keys, value_blocks = cut(queries), cut(keys), cut(values)
    cumulative = jnp.cumsum(decays, axis=-1)
    ending = cumulative[..., -1:]
    gaps = cumulative[..., :, None] - cumulative[..., None, :]
    causal = jnp.arange(BLOCK_LEN)[:, None] >= jnp.arange(BLOCK_LEN)[None, :]
    weighting = jnp.where(causal, jnp.exp(jnp.minimum(gaps, 0.0)), 0.0)
    decayed_keys = (keys.astype(jnp.float32) * jnp.exp(ending - cumulative)[..., None]).astype(
        jnp.bfloat16
    )
    block_kv = jnp.einsum(
        "bnjd,bnje->bnde", decayed_keys, value_blocks, preferred_element_type=jnp.float32
    )
    state = jnp.zeros_like(block_kv[:, 0])
    start = jnp.zeros_like(ending[:, 0])
    before, starts = [], []
    for n in range(blocks):
        before.append(state)
        starts.append(start)
        state = state * jnp.exp(ending[:, n])[..., None] + block_kv[:, n]
        start = start + ending[:, n]
    product = gate_c.astype(jnp.float32) * conv_in.astype(jnp.float32)
    halo = CONV_TAPS - 1
    packed = jnp.concatenate(
        [
            state,
            product[:, tok_rows - halo :],
            jnp.broadcast_to(start[..., None], (n_fs, 8 - halo, state.shape[-1])),
        ],
        axis=1,
    )
    shared = lax.all_gather(packed, "sp")
    state_in = jnp.zeros_like(state)
    rim = jnp.zeros_like(product[:, :halo])
    for k in range(n_sp - 1):
        part, total = shared[k, :, :KEY_DIM], shared[k, :, KEY_DIM + halo :][:, :1, :1]
        state_in = jnp.where(k < s, state_in * jnp.exp(total) + part, state_in)
        rim = jnp.where(k == s - 1, shared[k, :, KEY_DIM : KEY_DIM + halo], rim)

    raw = jnp.einsum("bnid,bnjd->bnij", queries, keys, preferred_element_type=jnp.float32)
    scores = (raw * weighting).astype(jnp.bfloat16)
    intra = jnp.einsum("bnij,bnje->bnie", scores, value_blocks, preferred_element_type=jnp.float32)
    decayed_queries = (queries.astype(jnp.float32) * jnp.exp(cumulative)[..., None]).astype(
        jnp.bfloat16
    )
    full_states = (
        jnp.stack(before, axis=1) + jnp.exp(jnp.stack(starts, axis=1))[..., None] * state_in[:, None]
    )
    cross = jnp.einsum(
        "bnid,bnde->bnie",
        decayed_queries,
        full_states.astype(jnp.bfloat16),
        preferred_element_type=jnp.float32,
    )
    output = intra + cross
    output = output * lax.rsqrt(jnp.mean(output * output, axis=-1, keepdims=True) + EPSILON)
    output = output.reshape(n_fs, tok_rows, values.shape[-1])
    ret_out = (output * jax.nn.silu(ret_gate.astype(jnp.float32))).astype(jnp.bfloat16)

    padded = jnp.concatenate([rim, product], axis=1)
    width = product.shape[-1]
    taps = lax.dynamic_slice_in_dim(conv_kernel, f * width, width, axis=1)
    convolved = sum(taps[k] * padded[:, k : k + tok_rows] for k in range(CONV_TAPS))
    conv_out = (gate_b.astype(jnp.float32) * convolved).astype(jnp.bfloat16)

    same, cross_core, far_weight = swap(jnp.concatenate([ret_out, conv_out], axis=-1), out_weight)

    def spread(piece):
        parts = piece.reshape(n_fs, half, 2, width)
        return jnp.transpose(parts, (1, 2, 0, 3)).reshape(half, 2 * n_fs * width)

    def project(piece, weight):
        return lax.dot_general(
            spread(piece), weight, (((1,), (1,)), ((), ())), preferred_element_type=jnp.float32
        )

    mixed = project(same, out_weight) + project(cross_core, far_weight)
    return mixed.astype(jnp.bfloat16)[None]


def select(mesh):
    def chosen(*arrays):
        heads, conv_width = arrays[12].shape[1], arrays[9].shape[1]
        n_sp, n_fs, n_tp = (mesh.shape[name] for name in ("sp", "fs", "tp"))
        fits = n_fs == 4 and n_tp == 2 and n_sp > 1 and heads == n_fs
        fits = fits and conv_width == n_fs * VALUE_DIM and arrays[0].shape[1] % (2 * BLOCK_LEN) == 0
        return (fast_shards if fits else shards)(*arrays)

    return chosen


def solution(mesh):
    in_specs = (
        P("fs", "sp", None),
        P(),
        P(("sp", "fs"), "tp"),
        P(("sp", "fs"), "tp"),
        P(("sp", "fs"), "tp"),
        P(("sp", "fs"), "tp"),
        P(("sp", "fs"), "tp"),
        P(("sp", "fs"), "tp"),
        P(("sp", "fs"), "tp"),
        P(None, "tp"),
        P(("sp", "fs"), "tp"),
        P(("sp", "fs"), "tp"),
        P("fs", "tp", "sp"),
    )
    out_specs = P("fs", ("sp", "tp"), None)
    return jax.shard_map(select(mesh), mesh=mesh, in_specs=in_specs, out_specs=out_specs, check_vma=False)
```

```python
import jax
import jax.numpy as jnp
from jax import lax
from jax.experimental import pallas as pl
from jax.experimental.pallas import tpu as pltpu
from jax.sharding import PartitionSpec as P

KEY_DIM = 64
VALUE_DIM = 128
CONV_TAPS = 3
BLOCK_LEN = 128


EPSILON = 1e-06
ROPE_BASE = 10000.0


def entering(x, axis, combine, identity):
    length, here = (lax.axis_size(axis), lax.axis_index(axis))
    everything = jax.tree.map(
        lambda part, kind: lax.all_gather(part.astype(kind), axis), x, (jnp.bfloat16, jnp.bfloat16)
    )
    start = jax.tree.map(
        lambda part, zero: jnp.broadcast_to(jnp.asarray(zero, part.dtype), part.shape), x, identity
    )

    def lap(k, before):
        reached = k < here
        new = combine(
            before, jax.tree.map(lambda part, own: part[k].astype(own.dtype), everything, x)
        )
        return jax.tree.map(lambda a, b: jnp.where(reached, a, b), new, before)

    return lax.fori_loop(0, length, lap, start)


def passed_along(value, axis, steps):
    count = lax.axis_size(axis)
    first, last = (max(0, -steps), min(count, count - steps))
    return lax.ppermute(value, axis, [(source, source + steps) for source in range(first, last)])


def rotate(values, token_ordinal):
    half_dim = values.shape[-1] // 2
    frequency = 1.0 / ROPE_BASE ** jnp.linspace(0.0, 1.0, half_dim, dtype=jnp.float32)
    angles = token_ordinal[:, None] * frequency[None, :]
    cosine_table = jnp.cos(angles)[:, None, :]
    sine_table = jnp.sin(angles)[:, None, :]
    first = values[..., :half_dim].astype(jnp.float32)
    second = values[..., half_dim:].astype(jnp.float32)
    return jnp.concatenate(
        [first * cosine_table - second * sine_table, first * sine_table + second * cosine_table],
        axis=-1,
    )


def make_adder(normed, contracted, pieces):
    updated = []
    for member in range(len(pieces)):
        portion = pieces[member]
        if member < contracted:
            updated.append(jnp.dot(normed, portion, preferred_element_type=jnp.float32))
        else:
            updated.append(portion)
    return tuple(updated)


def retention_local(projections, decays, token_ordinal):
    tok_rows = token_ordinal.shape[0]
    head_count = decays.shape[0]
    blocks = tok_rows // BLOCK_LEN
    query_raw = projections[0].reshape(tok_rows, head_count, KEY_DIM)
    key_raw = projections[1].reshape(tok_rows, head_count, KEY_DIM)
    queries = rotate(query_raw, token_ordinal).astype(jnp.bfloat16)
    lookup_matrix_lines = (rotate(key_raw, token_ordinal) * KEY_DIM ** (-0.5)).astype(jnp.bfloat16)
    value_proj = projections[2].reshape(tok_rows, head_count, VALUE_DIM)

    def split_blocks(array):
        shaped = array.reshape(blocks, BLOCK_LEN, head_count, array.shape[-1])
        return jnp.transpose(shaped, (0, 2, 1, 3))

    query_blocks = split_blocks(queries)
    key_blocks = split_blocks(lookup_matrix_lines)
    value_blocks = split_blocks(value_proj)
    decay_blocks = jnp.transpose(decays.reshape(head_count, blocks, BLOCK_LEN), (1, 0, 2))
    cumulative = jnp.cumsum(decay_blocks, axis=-1)
    ending = cumulative[..., -1:]
    decay_gaps = cumulative[..., :, None] - cumulative[..., None, :]
    causal = jnp.arange(BLOCK_LEN)[:, None] >= jnp.arange(BLOCK_LEN)[None, :]
    weighting = jnp.where(causal, jnp.exp(jnp.minimum(decay_gaps, 0.0)), 0.0)
    raw_scores = jnp.einsum(
        "nhid,nhjd->nhij", query_blocks, key_blocks, preferred_element_type=jnp.float32
    )
    scores = (raw_scores * weighting).astype(jnp.bfloat16)
    intra_out = jnp.einsum(
        "nhij,nhje->nhie", scores, value_blocks, preferred_element_type=jnp.float32
    )
    decayed_keys = (
        key_blocks.astype(jnp.float32) * jnp.exp(ending - cumulative)[..., None]
    ).astype(jnp.bfloat16)
    decayed_queries = (query_blocks.astype(jnp.float32) * jnp.exp(cumulative)[..., None]).astype(
        jnp.bfloat16
    )
    block_kv = jnp.einsum(
        "nhjd,nhje->nhde", decayed_keys, value_blocks, preferred_element_type=jnp.float32
    )
    block_ends = ending[..., 0]

    def advance(state_now, step_in):
        kv_block, total = step_in
        return (state_now * jnp.exp(total)[:, None, None] + kv_block, state_now)

    start_state = jnp.zeros((head_count, KEY_DIM, VALUE_DIM), jnp.float32)
    end_state, before_local = lax.scan(advance, start_state, (block_kv, block_ends))
    device_total = jnp.sum(block_ends, axis=0)
    return (intra_out, decayed_queries, before_local, block_ends, end_state, device_total)


def combine(earlier, later):
    return (earlier[0] * jnp.exp(later[1])[:, None, None] + later[0], earlier[1] + later[1])


def carried(end_state, device_total):
    identity = (jnp.zeros_like(end_state), jnp.zeros_like(device_total))
    state_in, _ = entering((end_state, device_total), "sp", combine, identity)
    return state_in


def retention_finish(local_parts, state_in, gate_proj):
    intra_out, decayed_queries, before_local, block_ends, end_state, device_total = local_parts
    starts = jnp.cumsum(block_ends, axis=0) - block_ends
    full_states = before_local + jnp.exp(starts)[:, :, None, None] * state_in[None]
    cross = jnp.einsum(
        "nhid,nhde->nhie",
        decayed_queries,
        full_states.astype(jnp.bfloat16),
        preferred_element_type=jnp.float32,
    )
    output = intra_out + cross
    output = output * lax.rsqrt(jnp.mean(output * output, axis=-1, keepdims=True) + EPSILON)
    tok_rows = gate_proj.shape[0]
    output = jnp.transpose(output, (0, 2, 1, 3)).reshape(tok_rows, gate_proj.shape[1])
    return (output * jax.nn.silu(gate_proj.astype(jnp.float32))).astype(jnp.bfloat16)


def convolve(conv_proj, conv_kernel):
    gate_b, gate_c, conv_input = conv_proj
    tok_rows = gate_b.shape[0]
    product = gate_c.astype(jnp.float32) * conv_input.astype(jnp.float32)
    rim_rows = passed_along(product[tok_rows - (CONV_TAPS - 1) :], "sp", 1)
    padded = jnp.concatenate([rim_rows, product], axis=0)
    convolved = jnp.zeros_like(product)
    for tap_index in range(CONV_TAPS):
        convolved = convolved + conv_kernel[tap_index] * padded[tap_index : tap_index + tok_rows]
    return (gate_b.astype(jnp.float32) * convolved).astype(jnp.bfloat16)


def shards(
    tokens,
    norm_gain,
    query_weight,
    key_weight,
    value_weight,
    gate_weight,
    conv_b_weight,
    conv_c_weight,
    conv_in_weight,
    conv_kernel,
    out_ret_weight,
    out_conv_weight,
    log_decay,
):
    inputs = tokens[0].astype(jnp.float32)
    tok_rows = inputs.shape[0]
    normed = (
        inputs * lax.rsqrt(jnp.mean(inputs * inputs, axis=-1, keepdims=True) + EPSILON) * norm_gain
    ).astype(jnp.bfloat16)
    token_ordinal = (
        lax.axis_index("sp") * tok_rows + jnp.arange(tok_rows, dtype=jnp.int32)
    ).astype(jnp.float32)
    decays = log_decay[0]
    gathered = make_adder(
        normed,
        7,
        (
            lax.all_gather(query_weight, ("sp", "fs"), axis=0, tiled=True),
            lax.all_gather(key_weight, ("sp", "fs"), axis=0, tiled=True),
            lax.all_gather(value_weight, ("sp", "fs"), axis=0, tiled=True),
            lax.all_gather(gate_weight, ("sp", "fs"), axis=0, tiled=True),
            lax.all_gather(conv_b_weight, ("sp", "fs"), axis=0, tiled=True),
            lax.all_gather(conv_c_weight, ("sp", "fs"), axis=0, tiled=True),
            lax.all_gather(conv_in_weight, ("sp", "fs"), axis=0, tiled=True),
            lax.all_gather(out_ret_weight, ("sp", "fs"), axis=0, tiled=True),
            lax.all_gather(out_conv_weight, ("sp", "fs"), axis=0, tiled=True),
        ),
    )
    ret_proj = [member.astype(jnp.bfloat16) for member in gathered[:4]]
    local_parts = retention_local(ret_proj, decays, token_ordinal)
    state_in = carried(local_parts[4], local_parts[5])
    conv_proj = [member.astype(jnp.bfloat16) for member in gathered[4:7]]
    full_ret, full_conv = (gathered[7], gathered[8])
    conv_out = convolve(conv_proj, conv_kernel)
    ret_out = retention_finish(local_parts, state_in, ret_proj[3])
    partial_value = lax.dot_general(
        ret_out, full_ret, (((1,), (1,)), ((), ())), preferred_element_type=jnp.float32
    )
    mixed = lax.psum_scatter(
        (
            partial_value
            + lax.dot_general(
                conv_out, full_conv, (((1,), (1,)), ((), ())), preferred_element_type=jnp.float32
            )
        ).astype(jnp.bfloat16),
        "tp",
        scatter_dimension=0,
        tiled=True,
    )
    return mixed[None]


MESH_IDS = pl.DeviceIdType.MESH


def remote(source, target, sent, landed, device):
    return pltpu.make_async_remote_copy(
        src_ref=source,
        dst_ref=target,
        send_sem=sent,
        recv_sem=landed,
        device_id=device,
        device_id_type=MESH_IDS,
    )


def greet(peers):
    barrier = pltpu.get_barrier_semaphore()
    for peer in peers:
        pl.semaphore_signal(barrier, inc=1, device_id=peer, device_id_type=MESH_IDS)
    pl.semaphore_wait(barrier, len(peers))


def plane_partners(f):
    x, y = f % 2, f // 2
    return y * 2 + (1 - x), (1 - y) * 2 + x, 3 - f


def gather_kernel(
    n_sp,
    half_ref,
    weight_ref,
    decay_ref,
    out_ref,
    proj_ref,
    decays_ref,
    outs_ref,
    normed_ref,
    full_ref,
    norm_sent,
    norm_landed,
    side_sent,
    side_landed,
    relay_sent,
    weight_sent,
    weight_landed,
    up_sent,
    down_sent,
    line_landed,
    decay_sent,
    decay_landed,
    local_sem,
    out_up_sent,
    out_down_sent,
    out_line_landed,
    out_plane_sent,
    out_plane_landed,
    out_relay_sent,
):
    s, f, t = lax.axis_index("sp"), lax.axis_index("fs"), lax.axis_index("tp")
    xn, yn, dn = plane_partners(f)
    half = half_ref.shape[0]
    chunk = half // 2
    rows = weight_ref.shape[1]
    n_fs = weight_ref.shape[0]
    other = {"tp": 1 - t}
    peers = [{"fs": xn}, {"fs": yn}, {"fs": dn}, other]
    peers += [{"sp": (s + d) % n_sp} for d in range(1, n_sp)]
    greet(peers)

    def spot(owner, core, piece):
        return normed_ref.at[owner, pl.ds(core * half + piece * chunk, chunk), :]

    def own(piece):
        return half_ref.at[pl.ds(piece * chunk, chunk), :]

    def outs(b, g):
        return outs_ref.at[pl.ds((b * n_fs + g) * rows, rows), :]

    def block(b, g):
        return full_ref.at[pl.ds((b * n_fs + g) * rows, rows), :]

    waits = []
    locals_ = []

    def start(copy):
        copy.start()
        waits.append(copy)

    order = (xn, yn, dn)
    for i, p in enumerate(order):
        start(remote(weight_ref.at[p], block(s, f), weight_sent.at[i], weight_landed.at[f], {"fs": p}))
    for i, p in enumerate(order):
        start(remote(decay_ref.at[p], decays_ref.at[f], decay_sent.at[i], decay_landed.at[f], {"fs": p}))
    start(remote(own(0), spot(f, t, 0), norm_sent.at[0], norm_landed.at[f, 0], {"fs": xn}))
    start(remote(own(1), spot(f, t, 1), norm_sent.at[1], norm_landed.at[f, 1], {"fs": yn}))
    start(remote(own(1), spot(f, t, 1), norm_sent.at[2], norm_landed.at[f, 1], {"fs": xn}))
    start(remote(own(0), spot(f, t, 0), norm_sent.at[3], norm_landed.at[f, 0], {"fs": yn}))

    def line_copy(source, b, g, way):
        sent = up_sent if way == 1 else down_sent
        return remote(source, block(b, g), sent.at[b, g], line_landed.at[b, g], {"sp": s + way})

    def send_line(source, b, g):
        @pl.when(s < n_sp - 1)
        def _():
            line_copy(source, b, g, 1).start()

        @pl.when(s > 0)
        def _():
            line_copy(source, b, g, -1).start()

    def out_line(source, b, way):
        sent = out_up_sent if way == 1 else out_down_sent
        return remote(source, outs(b, f), sent.at[b], out_line_landed.at[b], {"sp": s + way})

    def out_plane(source, b, i):
        return remote(
            source, outs(b, f), out_plane_sent.at[b, i], out_plane_landed.at[b, f], {"fs": order[i]}
        )

    send_line(weight_ref.at[f], s, f)

    @pl.when(s < n_sp - 1)
    def _():
        out_line(out_ref, s, 1).start()

    @pl.when(s > 0)
    def _():
        out_line(out_ref, s, -1).start()

    for piece in range(2):
        start(remote(own(piece), spot(f, t, piece), side_sent.at[f, piece], side_landed.at[f, piece], other))
    for i, (a, b) in enumerate(
        (
            (own(0), spot(f, t, 0)),
            (own(1), spot(f, t, 1)),
            (weight_ref.at[f], block(s, f)),
            (decay_ref.at[f], decays_ref.at[f]),
            (out_ref, outs(s, f)),
        )
    ):
        copy = pltpu.make_async_copy(a, b, local_sem.at[i])
        copy.start()
        locals_.append(copy)

    for p in order:
        remote(weight_ref.at[p], block(s, p), weight_sent.at[0], weight_landed.at[p], {"fs": p}).wait_recv()
        send_line(block(s, p), s, p)

    for i in range(2):
        out_plane(out_ref, s, i).start()

    def arrived(owner, piece):
        view = spot(owner, t, piece)
        remote(view, view, norm_sent.at[0], norm_landed.at[owner, piece], {"fs": owner}).wait_recv()
        start(remote(view, view, side_sent.at[owner, piece], side_landed.at[owner, piece], other))

    def line_step(d):
        for g in (f,) + order:

            @pl.when(s - d >= 0)
            def _():
                line_copy(block(s - d, g), s - d, g, 1).wait_recv()

                @pl.when(s < n_sp - 1)
                def _():
                    line_copy(block(s - d, g), s - d, g, 1).start()

            @pl.when(s + d <= n_sp - 1)
            def _():
                line_copy(block(s + d, g), s + d, g, -1).wait_recv()

                @pl.when(s > 0)
                def _():
                    line_copy(block(s + d, g), s + d, g, -1).start()

    def out_step(d):
        for b, way, there, further in (
            (s - d, 1, s - d >= 0, s < n_sp - 1),
            (s + d, -1, s + d <= n_sp - 1, s > 0),
        ):

            @pl.when(there)
            def _():
                out_line(outs(b, f), b, way).wait_recv()

                @pl.when(further)
                def _():
                    out_line(outs(b, f), b, way).start()

                for i in range(2):
                    out_plane(outs(b, f), b, i).start()

    arrived(xn, 0)
    start(remote(spot(xn, t, 0), spot(xn, t, 0), relay_sent.at[0], norm_landed.at[xn, 0], {"fs": yn}))
    arrived(yn, 1)
    start(remote(spot(yn, t, 1), spot(yn, t, 1), relay_sent.at[1], norm_landed.at[yn, 1], {"fs": xn}))
    line_step(1)
    out_step(1)
    arrived(xn, 1)
    arrived(yn, 0)
    for d in range(2, n_sp - 1):
        line_step(d)
        out_step(d)
    arrived(dn, 0)
    arrived(dn, 1)
    if n_sp > 2:
        line_step(n_sp - 1)
        out_step(n_sp - 1)
    for p in order:
        remote(decay_ref.at[p], decays_ref.at[p], decay_sent.at[0], decay_landed.at[p], {"fs": p}).wait_recv()
    for owner in range(n_fs):
        for piece in range(2):
            view = spot(owner, 1 - t, piece)
            remote(view, view, side_sent.at[0, 0], side_landed.at[owner, piece], other).wait_recv()
    for copy in locals_:
        copy.wait()

    def out_landed(b, g):
        remote(outs(b, g), outs(b, g), out_relay_sent.at[0], out_plane_landed.at[b, g], {"fs": g}).wait_recv()

    for b in range(n_sp):
        g, onward = (xn, yn) if b < n_sp // 2 else (yn, xn)
        out_landed(b, g)
        start(
            remote(outs(b, g), outs(b, g), out_relay_sent.at[b], out_plane_landed.at[b, g], {"fs": onward})
        )

    tile = chunk
    tiles = 2 * half // tile

    @pl.loop(0, n_fs * tiles)
    def _(step):
        owner, at = step // tiles, pl.ds((step % tiles) * tile, tile)
        proj_ref[owner, at, :] = jnp.dot(
            normed_ref[owner, at, :], full_ref[...], preferred_element_type=jnp.float32
        ).astype(jnp.bfloat16)

    for b in range(n_sp):
        out_landed(b, yn if b < n_sp // 2 else xn)
        out_landed(b, dn)
    for copy in waits:
        copy.wait_send()
    for b in range(n_sp):
        for i in range(2):
            out_plane(outs(b, f), b, i).wait_send()

        @pl.when((s < n_sp - 1) & (b <= s))
        def _():
            out_line(outs(b, f), b, 1).wait_send()

        @pl.when((s > 0) & (b >= s))
        def _():
            out_line(outs(b, f), b, -1).wait_send()

    for b in range(n_sp):
        for g in range(n_fs):

            @pl.when((s < n_sp - 1) & (b <= s))
            def _():
                line_copy(block(b, g), b, g, 1).wait_send()

            @pl.when((s > 0) & (b >= s))
            def _():
                line_copy(block(b, g), b, g, -1).wait_send()


def gather_all(n_sp, half, pieces, decays, own_out):
    n_fs, rows, width = pieces.shape
    any_space = pl.BlockSpec(memory_space=pl.ANY)
    vmem = pl.BlockSpec(memory_space=pltpu.VMEM)
    dma = pltpu.SemaphoreType.DMA
    return pl.pallas_call(
        lambda *refs: gather_kernel(n_sp, *refs),
        out_shape=(
            jax.ShapeDtypeStruct((n_fs, 2 * half.shape[0], width), jnp.bfloat16),
            jax.ShapeDtypeStruct(decays.shape, jnp.float32),
            jax.ShapeDtypeStruct((n_sp * n_fs * rows, own_out.shape[1]), jnp.bfloat16),
        ),
        in_specs=[vmem] * 4,
        out_specs=(vmem, vmem, any_space),
        scratch_shapes=[
            pltpu.VMEM((n_fs, 2 * half.shape[0], half.shape[1]), jnp.bfloat16),
            pltpu.VMEM((n_sp * n_fs * rows, width), jnp.bfloat16),
            dma((4,)),
            dma((n_fs, 2)),
            dma((n_fs, 2)),
            dma((n_fs, 2)),
            dma((2,)),
            dma((3,)),
            dma((n_fs,)),
            dma((n_sp, n_fs)),
            dma((n_sp, n_fs)),
            dma((n_sp, n_fs)),
            dma((3,)),
            dma((n_fs,)),
            dma((5,)),
            dma((n_sp,)),
            dma((n_sp,)),
            dma((n_sp,)),
            dma((n_sp, 2)),
            dma((n_sp, n_fs)),
            dma((n_sp,)),
        ],
        compiler_params=pltpu.CompilerParams(collective_id=0, has_side_effects=True),
        cost_estimate=pl.CostEstimate(flops=0, bytes_accessed=200_000_000, transcendentals=0),
        name="gather_all",
    )(half, pieces, decays, own_out)


def swap_kernel(
    mixed_ref, weight_ref, same_ref, cross_ref, far_ref, sent, same_landed, cross_landed, weight_sems, local_sem
):
    f, t = lax.axis_index("fs"), lax.axis_index("tp")
    half = same_ref.shape[1]
    order = plane_partners(f)
    peers = [{"fs": p, "tp": q} for p in order for q in (t, 1 - t)] + [{"tp": 1 - t}]
    greet(peers)

    def mine(p, core):
        return mixed_ref.at[p, pl.ds(core * half, half), :]

    copies = []
    for i, p in enumerate((order[2], order[0], order[1])):
        copies.append(
            remote(mine(p, t), same_ref.at[f], sent.at[2 * i], same_landed.at[f], {"fs": p})
        )
        copies.append(
            remote(
                mine(p, 1 - t),
                cross_ref.at[f],
                sent.at[2 * i + 1],
                cross_landed.at[f],
                {"fs": p, "tp": 1 - t},
            )
        )
    copies.append(remote(mine(f, 1 - t), cross_ref.at[f], sent.at[6], cross_landed.at[f], {"tp": 1 - t}))
    for copy in copies:
        copy.start()
    weight = remote(weight_ref, far_ref, weight_sems.at[0], weight_sems.at[1], {"tp": 1 - t})
    weight.start()
    local = pltpu.make_async_copy(mine(f, t), same_ref.at[f], local_sem)
    local.start()
    for p in order:
        remote(same_ref.at[p], same_ref.at[p], sent.at[0], same_landed.at[p], {"fs": p}).wait_recv()
    for p in order + (f,):
        remote(cross_ref.at[p], cross_ref.at[p], sent.at[0], cross_landed.at[p], {"tp": 1 - t}).wait_recv()
    for copy in copies:
        copy.wait_send()
    local.wait()
    weight.wait()


def swap(mixed, weight):
    n_fs, rows, width = mixed.shape
    any_space = pl.BlockSpec(memory_space=pl.ANY)
    vmem = pl.BlockSpec(memory_space=pltpu.VMEM)
    dma = pltpu.SemaphoreType.DMA
    piece = jax.ShapeDtypeStruct((n_fs, rows // 2, width), jnp.bfloat16)
    return pl.pallas_call(
        swap_kernel,
        out_shape=(piece, piece, jax.ShapeDtypeStruct(weight.shape, weight.dtype)),
        in_specs=[vmem, any_space],
        out_specs=(vmem, vmem, any_space),
        scratch_shapes=[dma((7,)), dma((n_fs,)), dma((n_fs,)), dma((2,)), dma],
        compiler_params=pltpu.CompilerParams(collective_id=1, has_side_effects=True),
        cost_estimate=pl.CostEstimate(flops=0, bytes_accessed=60_000_000, transcendentals=0),
        name="swap",
    )(mixed, weight)


def pass_kernel(n_sp, state_ref, extra_ref, states_ref, extras_ref, sent, landed, local_sem):
    s = lax.axis_index("sp")
    greet([{"sp": (s + d) % n_sp} for d in range(1, n_sp)])

    def pair(source, here, owner, d):
        place = here.at[owner]
        slot = 0 if source is state_ref else 1
        return remote(source, place, sent.at[d, slot], landed.at[owner, slot], {"sp": (s + d) % n_sp})

    arrays = ((state_ref, states_ref), (extra_ref, extras_ref))
    for d in range(n_sp - 1, 0, -1):

        @pl.when(s + d < n_sp)
        def _():
            for source, here in arrays:
                pair(source, here, s, d).start()

    states_ref[n_sp - 1] = jnp.zeros_like(state_ref)
    extras_ref[n_sp - 1] = jnp.zeros_like(extra_ref)
    for k in range(n_sp - 1):

        @pl.when(k < s)
        def _():
            for source, here in arrays:
                pair(source, here, k, 1).wait_recv()

        @pl.when(k >= s)
        def _():
            states_ref[k] = jnp.zeros_like(state_ref)
            extras_ref[k] = jnp.zeros_like(extra_ref)

    for d in range(1, n_sp):

        @pl.when(s + d < n_sp)
        def _():
            for source, here in arrays:
                pair(source, here, s, d).wait_send()


def pass_on(n_sp, state, extra):
    vmem = pl.BlockSpec(memory_space=pltpu.VMEM)
    dma = pltpu.SemaphoreType.DMA
    return pl.pallas_call(
        lambda *refs: pass_kernel(n_sp, *refs),
        out_shape=(
            jax.ShapeDtypeStruct((n_sp,) + state.shape, state.dtype),
            jax.ShapeDtypeStruct((n_sp,) + extra.shape, extra.dtype),
        ),
        in_specs=[vmem] * 2,
        out_specs=(vmem, vmem),
        scratch_shapes=[dma((n_sp, 2)), dma((n_sp, 2)), dma],
        compiler_params=pltpu.CompilerParams(collective_id=2, has_side_effects=True),
        cost_estimate=pl.CostEstimate(flops=0, bytes_accessed=20_000_000, transcendentals=0),
        name="pass_on",
    )(state, extra)


def rotate_flat(values, cosine, sine):
    half_dim = values.shape[-1] // 2
    first = values[..., :half_dim].astype(jnp.float32)
    second = values[..., half_dim:].astype(jnp.float32)
    return jnp.concatenate([first * cosine - second * sine, first * sine + second * cosine], axis=-1)


def fast_shards(
    tokens,
    norm_gain,
    query_weight,
    key_weight,
    value_weight,
    gate_weight,
    conv_b_weight,
    conv_c_weight,
    conv_in_weight,
    conv_kernel,
    out_ret_weight,
    out_conv_weight,
    log_decay,
):
    n_sp, n_fs = lax.axis_size("sp"), lax.axis_size("fs")
    s, f, t = lax.axis_index("sp"), lax.axis_index("fs"), lax.axis_index("tp")
    tok_rows, model = tokens.shape[1:]
    half = tok_rows // 2
    blocks = tok_rows // BLOCK_LEN
    rows = query_weight.shape[0]
    inputs = lax.dynamic_slice_in_dim(tokens[0], t * half, half).astype(jnp.float32)
    normed = (
        inputs * lax.rsqrt(jnp.mean(inputs * inputs, axis=-1, keepdims=True) + EPSILON) * norm_gain
    ).astype(jnp.bfloat16)
    pieces = jnp.concatenate(
        [
            jnp.transpose(w.reshape(rows, n_fs, w.shape[1] // n_fs), (1, 0, 2))
            for w in (
                query_weight,
                key_weight,
                value_weight,
                gate_weight,
                conv_b_weight,
                conv_c_weight,
                conv_in_weight,
            )
        ],
        axis=-1,
    )
    own_out = jnp.concatenate([out_ret_weight, out_conv_weight], axis=-1)
    proj, decays, out_weight = gather_all(
        n_sp, normed, pieces, log_decay[0].reshape(n_fs, blocks, BLOCK_LEN), own_out
    )
    cuts = (KEY_DIM, 2 * KEY_DIM)
    q_raw, k_raw, wide = proj[..., : cuts[0]], proj[..., cuts[0] : cuts[1]], proj[..., cuts[1] :]
    values, ret_gate, gate_b, gate_c, conv_in = jnp.split(wide, 5, axis=-1)

    ordinal = (s * tok_rows + jnp.arange(tok_rows, dtype=jnp.int32)).astype(jnp.float32)
    frequency = 1.0 / ROPE_BASE ** jnp.linspace(0.0, 1.0, KEY_DIM // 2, dtype=jnp.float32)
    angles = ordinal[:, None] * frequency[None, :]
    cosine, sine = jnp.cos(angles), jnp.sin(angles)
    queries = rotate_flat(q_raw, cosine, sine).astype(jnp.bfloat16)
    keys = (rotate_flat(k_raw, cosine, sine) * KEY_DIM ** (-0.5)).astype(jnp.bfloat16)

    def cut(array):
        return array.reshape(n_fs, blocks, BLOCK_LEN, array.shape[-1])

    queries, keys, value_blocks = cut(queries), cut(keys), cut(values)
    cumulative = jnp.cumsum(decays, axis=-1)
    ending = cumulative[..., -1:]
    gaps = cumulative[..., :, None] - cumulative[..., None, :]
    causal = jnp.arange(BLOCK_LEN)[:, None] >= jnp.arange(BLOCK_LEN)[None, :]
    weighting = jnp.where(causal, jnp.exp(jnp.minimum(gaps, 0.0)), 0.0)
    decayed_keys = (keys.astype(jnp.float32) * jnp.exp(ending - cumulative)[..., None]).astype(
        jnp.bfloat16
    )
    block_kv = jnp.einsum(
        "bnjd,bnje->bnde", decayed_keys, value_blocks, preferred_element_type=jnp.float32
    )
    state = jnp.zeros_like(block_kv[:, 0])
    start = jnp.zeros_like(ending[:, 0])
    before, starts = [], []
    for n in range(blocks):
        before.append(state)
        starts.append(start)
        state = state * jnp.exp(ending[:, n])[..., None] + block_kv[:, n]
        start = start + ending[:, n]
    product = gate_c.astype(jnp.float32) * conv_in.astype(jnp.float32)
    halo = CONV_TAPS - 1
    extra = jnp.concatenate(
        [
            product[:, tok_rows - halo :],
            jnp.broadcast_to(start[..., None], (n_fs, 8 - halo, product.shape[-1])),
        ],
        axis=1,
    )
    all_states, extras = pass_on(n_sp, state.astype(jnp.bfloat16), extra)
    state_in = jnp.zeros_like(state)
    rim = jnp.zeros_like(product[:, :halo])
    for k in range(n_sp - 1):
        part, total = all_states[k].astype(jnp.float32), extras[k, :, halo : halo + 1, :1]
        state_in = jnp.where(k < s, state_in * jnp.exp(total) + part, state_in)
        rim = jnp.where(k == s - 1, extras[k, :, :halo], rim)

    raw = jnp.einsum("bnid,bnjd->bnij", queries, keys, preferred_element_type=jnp.float32)
    scores = (raw * weighting).astype(jnp.bfloat16)
    intra = jnp.einsum("bnij,bnje->bnie", scores, value_blocks, preferred_element_type=jnp.float32)
    decayed_queries = (queries.astype(jnp.float32) * jnp.exp(cumulative)[..., None]).astype(
        jnp.bfloat16
    )
    full_states = (
        jnp.stack(before, axis=1) + jnp.exp(jnp.stack(starts, axis=1))[..., None] * state_in[:, None]
    )
    cross = jnp.einsum(
        "bnid,bnde->bnie",
        decayed_queries,
        full_states.astype(jnp.bfloat16),
        preferred_element_type=jnp.float32,
    )
    output = intra + cross
    output = output * lax.rsqrt(jnp.mean(output * output, axis=-1, keepdims=True) + EPSILON)
    output = output.reshape(n_fs, tok_rows, values.shape[-1])
    ret_out = (output * jax.nn.silu(ret_gate.astype(jnp.float32))).astype(jnp.bfloat16)

    padded = jnp.concatenate([rim, product], axis=1)
    width = product.shape[-1]
    taps = lax.dynamic_slice_in_dim(conv_kernel, f * width, width, axis=1)
    convolved = sum(taps[k] * padded[:, k : k + tok_rows] for k in range(CONV_TAPS))
    conv_out = (gate_b.astype(jnp.float32) * convolved).astype(jnp.bfloat16)

    same, cross_core, far_weight = swap(jnp.concatenate([ret_out, conv_out], axis=-1), out_weight)

    def spread(piece):
        parts = piece.reshape(n_fs, half, 2, width)
        return jnp.transpose(parts, (1, 2, 0, 3)).reshape(half, 2 * n_fs * width)

    def project(piece, weight):
        return lax.dot_general(
            spread(piece), weight, (((1,), (1,)), ((), ())), preferred_element_type=jnp.float32
        )

    mixed = project(same, out_weight) + project(cross_core, far_weight)
    return mixed.astype(jnp.bfloat16)[None]


def select(mesh):
    def chosen(*arrays):
        heads, conv_width = arrays[12].shape[1], arrays[9].shape[1]
        n_sp, n_fs, n_tp = (mesh.shape[name] for name in ("sp", "fs", "tp"))
        fits = n_fs == 4 and n_tp == 2 and n_sp > 1 and heads == n_fs
        fits = fits and conv_width == n_fs * VALUE_DIM and arrays[0].shape[1] % (2 * BLOCK_LEN) == 0
        return (fast_shards if fits else shards)(*arrays)

    return chosen


def solution(mesh):
    in_specs = (
        P("fs", "sp", None),
        P(),
        P(("sp", "fs"), "tp"),
        P(("sp", "fs"), "tp"),
        P(("sp", "fs"), "tp"),
        P(("sp", "fs"), "tp"),
        P(("sp", "fs"), "tp"),
        P(("sp", "fs"), "tp"),
        P(("sp", "fs"), "tp"),
        P(None, "tp"),
        P(("sp", "fs"), "tp"),
        P(("sp", "fs"), "tp"),
        P("fs", "tp", "sp"),
    )
    out_specs = P("fs", ("sp", "tp"), None)
    return jax.shard_map(select(mesh), mesh=mesh, in_specs=in_specs, out_specs=out_specs, check_vma=False)
```
